32 devices in a mesh: sp: 16 (over z, y, x), tp: 2 (over core).
Axes of the slice: x: 2, y: 2, z: 4, core: 2. Of those that a mesh axis runs over, the one named last changes fastest.
Arguments:
- stream: bfloat16 [4096, 2048], P('sp', 'tp'), may hold values from -80 to 80
- norm_gain: float32 [2048], P('tp'), may hold values from 0.1 to 1.9
- cotangent: bfloat16 [4096, 2048], P('sp', 'tp'), may hold values from -6 to 6
- route_weights: float32 [4096, 2], P('sp'), may hold values from 0.1 to 1.5
- routes: int32 [4096, 2], P('sp'), may hold values from 0 to 15, all different within a row; in each aligned block of 256 rows (0 to 255, 256 to 511, ...) at most 64 rows name the same one
- conv_input: bfloat16 [4096, 1024], P('sp', 'tp'), may hold values from -6 to 6
- conv_bgate: bfloat16 [4096, 1024], P('sp', 'tp'), may hold values from -6 to 6
- conv_cgate: bfloat16 [4096, 1024], P('sp', 'tp'), may hold values from -6 to 6
- conv_taps: float32 [3, 1024], P(None, 'tp'), may hold values from -3 to 3
- out_proj: bfloat16 [2048, 1024], P(None, 'tp'), may hold values from -0.1875 to 0.1875
- gate_weight: bfloat16 [16, 2048, 1024], P('sp', None, 'tp'), may hold values from -0.125 to 0.125
- up_weight: bfloat16 [16, 2048, 1024], P('sp', None, 'tp'), may hold values from -0.125 to 0.125
- down_weight: bfloat16 [16, 1024, 2048], P('sp', 'tp'), may hold values from -0.1875 to 0.1875
Outputs:
- stream_grad: bfloat16 [4096, 2048], P('sp', 'tp')
- proj_grad: float32 [2048, 1024], P('sp', 'tp')
- input_grad: bfloat16 [4096, 1024], P('sp', 'tp')
- bgate_grad: bfloat16 [4096, 1024], P('sp', 'tp')
- cgate_grad: bfloat16 [4096, 1024], P('sp', 'tp')
- gate_grad: float32 [16, 2048, 1024], P('sp', None, 'tp')
- up_grad: float32 [16, 2048, 1024], P('sp', None, 'tp')
- down_grad: float32 [16, 1024, 2048], P('sp', 'tp')
The draws below stay inside these ranges and needn't reach their ends.
Inputs may be any that keep to these rules, and one draw needn't show every extreme that they name: `routes`: the 2 experts of a token differ. Among the tokens of one index of sp, no expert is named more than 64 times, a bound that some block reaches.
All inputs are finite; a program needn't handle non-finite values.
Results may differ from the reference program's by a relative error of at most 0.003.
The reference program's roundings to bfloat16 on the way count: a program that leaves them out, or rounds other values in their place, can miss the bound.
Values may be sent and summed in bfloat16 or wider, within the bound.
A program may use at most 128 MiB of HBM per device.

```python
import math
import jax
import jax.numpy as jnp
import numpy as np
from jax import lax

D = 2048
CW = 1024
EH = 1024
K = 2
TOK_DEV = 256
TOKENS = 4096
EXPERTS = 16
CAP = 64
N_SP = 16
N_TP = 2


def draw_stream(key, part):
    keys = jax.random.split(key, 3)
    row_scale = jnp.exp(jax.random.uniform(keys[0], (TOKENS, 1), jnp.float32, 0.0, 2.3))
    column_rise = 3.0 ** (jnp.arange(D, dtype=jnp.float32) / D)
    column_scale = column_rise[None, :] * jnp.exp(jax.random.uniform(keys[1], (1, D), jnp.float32, -0.5, 0.5))
    values = jax.random.normal(keys[2], (TOKENS, D), jnp.float32)
    return jnp.clip(values * row_scale * column_scale, -80.0, 80.0).astype(jnp.bfloat16)


def spiked(array, key, source, target, parts, factor):
    def block_of(axis_at):
        return (jnp.arange(array.shape[axis_at]) // (array.shape[axis_at] // parts)).reshape((-1,) + (1,) * (array.ndim - 1 - axis_at))

    one_side = jax.random.permutation(key, parts)[block_of(target)]
    other_side = (block_of(target) + parts // 2) % parts
    return jnp.where((block_of(source) == one_side) | (block_of(source) == other_side), factor * array, array)


def steps_of(key, extent, shards, smallest, top_value):
    gain, own = 1.0, jax.random.fold_in(key, 6)
    for dim, parts in shards:
        steps = jnp.exp(jax.random.uniform(jax.random.fold_in(own, dim), (parts,), jnp.float32, smallest / len(shards), top_value / len(shards)))
        gain = gain * jnp.repeat(steps, extent[dim] // parts).reshape([-1 if axis == dim else 1 for axis in range(len(extent))])
    return gain


def shared_out(rng, own, number, rows, count, top, limit, slope):
    ranking = jax.random.permutation(rng, count)
    packed, ordinary = portions_of(count, rows * top, limit, slope, True), portions_of(count, rows * top, limit, slope, False)
    places = jnp.arange(count)

    def named(lengths, turn):
        used = int((lengths > 0).sum())
        fixed = max(1, used // 4)
        shifted = fixed + (places - fixed + turn * (used - fixed)) % max(1, count - fixed)
        return jnp.zeros((count,), jnp.int32).at[ranking[jnp.where(places < fixed, places, shifted)]].set(jnp.asarray(lengths, jnp.int32))

    lengths = jnp.where(number % 4 == 0, named(packed, number // 4), named(ordinary, number - number // 4 - 1))
    mixed = jax.random.permutation(jax.random.fold_in(own, 3), count)
    source_of, sink = mixed[0:count // 2 * 2:2], mixed[1:count // 2 * 2:2]
    room = jnp.minimum(lengths[source_of] - 1, limit - lengths[sink]) // 2
    room = jnp.where((source_of == ranking[0]) | (sink == ranking[0]) | (lengths[sink] == 0), 0, jnp.maximum(room, 0))
    shifted = jax.random.randint(jax.random.fold_in(own, 4), (count // 2,), 0, 1 << 20) % (room + 1)
    lengths = lengths.at[source_of].add(-shifted).at[sink].add(shifted)
    members = jnp.searchsorted(jnp.cumsum(lengths), jnp.arange(rows * top), side="right").astype(jnp.int32)
    grid = members.reshape(top, rows).T
    grid = grid[jax.random.permutation(jax.random.fold_in(own, 1), rows)]
    turn = jax.random.randint(jax.random.fold_in(own, 2), (rows, 1), 0, top)
    return jnp.take_along_axis(grid, (jnp.arange(top)[None, :] + turn) % top, axis=1)


def portions_of(amount, total, bound, lean, full):
    loads = [(1 << 20) // math.isqrt(standing ** lean) + 1 for standing in range(1, amount + 1)]
    largest = bound if full else min(bound, max(-(-total // amount), total * loads[0] // sum(loads)))
    least = 1 if total - largest >= amount - 1 else 0
    given, spare = [largest] + [least] * (amount - 1), total - largest - least * (amount - 1)
    while spare > 0:
        candidates = [i for i in range(1, amount) if given[i] < largest] or [i for i in range(1, amount) if given[i] < bound]
        mass, left = sum([loads[i] for i in candidates]), spare
        for i in candidates:
            extra = min(bound - given[i], max(1, left * loads[i] // mass), spare)
            given[i] = given[i] + extra
            spare = spare - extra
    return np.array(given)


def gaussian(stream_key, extent, spread, limit, pieces=(), kind=jnp.bfloat16):
    loudness = steps_of(stream_key, extent, pieces, -0.22, 0.18) if pieces else 1.0
    result = jax.random.normal(stream_key, extent, jnp.float32) * spread * loudness
    return jnp.minimum(jnp.maximum(result, -limit), limit).astype(kind)


def noise_with(own_key, extent, scale, bound, pieces, heavy, kind=jnp.bfloat16):
    entries = scale * jax.random.normal(own_key, extent, jnp.float32)
    if pieces:
        entries = entries * steps_of(own_key, extent, pieces, -0.22, 0.18)
    return jnp.clip(spiked(entries, jax.random.fold_in(own_key, 3), *heavy), -bound, bound).astype(kind)


def setup_inputs(seed: int = 0) -> dict:
    splits = jax.random.split(jax.random.key(seed), 14)
    stream = draw_stream(jax.random.fold_in(splits[13], 71), 0)
    norm_gain = jnp.clip(1.0 + 0.18 * jax.random.normal(splits[1], (D,), jnp.float32), 0.1, 1.9)
    cotangent = noise_with(splits[2], (TOKENS, D), 1.0, 6.0, ((0, 16), (1, 2)), (0, 1, 16, 2.0))
    route_weights = jnp.clip(0.1 + 1.4 * jax.random.uniform(splits[3], (TOKENS, K), jnp.float32) ** steps_of(splits[3], (TOKENS, K), ((0, 16),), -0.2, 0.2), 0.1, 1.5)
    routes_keys = jax.random.split(jax.random.fold_in(splits[4], 1), TOKENS // TOK_DEV)
    routes_turns = jax.random.permutation(jax.random.fold_in(splits[4], 3), TOKENS // TOK_DEV)
    routes = jax.vmap(lambda own, number: shared_out(jax.random.fold_in(splits[4], 2), own, number, TOK_DEV, EXPERTS, K, CAP, 1))(routes_keys, routes_turns).reshape((TOKENS, K))
    conv_input = gaussian(splits[5], (TOKENS, CW), 1.0, 6.0, ((0, 16), (1, 2)))
    conv_bgate = gaussian(splits[6], (TOKENS, CW), 1.0, 6.0, ((0, 16), (1, 2)))
    conv_cgate = gaussian(splits[7], (TOKENS, CW), 1.0, 6.0, ((0, 16), (1, 2)))
    conv_taps = gaussian(splits[8], (3, CW), 0.5, 3.0, ((1, 2),), jnp.float32)
    out_proj = gaussian(splits[9], (D, CW), CW ** -0.5, 0.1875, ((1, 2),))
    gate_weight = gaussian(splits[10], (EXPERTS, D, EH), D ** -0.5, 0.125, ((0, 16), (2, 2)))
    up_weight = gaussian(splits[11], (EXPERTS, D, EH), D ** -0.5, 0.125, ((0, 16), (2, 2)))
    down_weight = gaussian(splits[12], (EXPERTS, EH, D), EH ** -0.5, 0.1875, ((0, 16), (1, 2)))
    return {"stream": stream, "norm_gain": norm_gain, "cotangent": cotangent, "route_weights": route_weights, "routes": routes, "conv_input": conv_input, "conv_bgate": conv_bgate, "conv_cgate": conv_cgate, "conv_taps": conv_taps, "out_proj": out_proj, "gate_weight": gate_weight, "up_weight": up_weight, "down_weight": down_weight}


EPSILON = 1e-06

def expert_backward(inputs, grads_out, gate_w, up_w, down_w):
    gate_lin = jnp.dot(inputs, gate_w, preferred_element_type=jnp.float32)
    up_lin = jnp.dot(inputs, up_w, preferred_element_type=jnp.float32)
    sigmoid_gate = jax.nn.sigmoid(gate_lin)
    silu_gate = gate_lin * sigmoid_gate
    hidden = (silu_gate * up_lin).astype(jnp.bfloat16)
    down_g = jnp.dot(hidden.T, grads_out, preferred_element_type=jnp.float32)
    hidden_grad = jnp.dot(grads_out, down_w.T, preferred_element_type=jnp.float32)
    gate_pre = (hidden_grad * up_lin * sigmoid_gate * (1.0 + gate_lin * (1.0 - sigmoid_gate))).astype(jnp.bfloat16)
    up_pre = (hidden_grad * silu_gate).astype(jnp.bfloat16)
    gate_g = jnp.dot(inputs.T, gate_pre, preferred_element_type=jnp.float32)
    up_g = jnp.dot(inputs.T, up_pre, preferred_element_type=jnp.float32)
    return (gate_g, up_g, down_g, gate_pre, up_pre)

def reference(stream, norm_gain, cotangent, route_weights, routes, conv_input, conv_bgate, conv_cgate, conv_taps, out_proj, gate_weight, up_weight, down_weight):
    stream_float = stream.astype(jnp.float32)
    inverse = lax.rsqrt(lax.optimization_barrier(jnp.mean(stream_float * stream_float, axis=1, keepdims=True)) + EPSILON)
    normed = (stream_float * inverse * norm_gain[None, :]).astype(jnp.bfloat16)
    cot_float = cotangent.astype(jnp.float32)
    weighted = (route_weights[:, :, None] * cot_float[:, None, :]).astype(jnp.bfloat16).reshape(TOKENS * K, D)
    blocks = routes.reshape(N_SP, TOK_DEV * K).astype(jnp.int32)
    onehot = (blocks[:, :, None] == jnp.arange(EXPERTS, dtype=jnp.int32)[None, None, :]).astype(jnp.int32)
    earlier = jnp.cumsum(onehot, axis=1) - onehot
    position = lax.optimization_barrier(jnp.sum(earlier * onehot, axis=2)).astype(jnp.int32)
    source = jnp.arange(N_SP, dtype=jnp.int32)[:, None]
    arrival = (source * CAP + position).astype(jnp.int32)
    assign_ids = jnp.arange(TOKENS * K, dtype=jnp.int32).reshape(N_SP, TOK_DEV * K)
    table = jnp.full((EXPERTS, N_SP * CAP), TOKENS * K, jnp.int32).at[blocks, arrival].set(assign_ids)
    normed_pad = jnp.concatenate([normed, jnp.zeros((1, D), jnp.bfloat16)], axis=0)
    weighted_pad = jnp.concatenate([weighted, jnp.zeros((1, D), jnp.bfloat16)], axis=0)
    half_width = EH // N_TP

    def one_expert(operands):
        slot_ids, gate_w, up_w, down_w = operands
        token_ids = (slot_ids // K).astype(jnp.int32)
        inputs = normed_pad[token_ids]
        grads_out = weighted_pad[slot_ids]
        gate_g, up_g, down_g, gate_pre, up_pre = expert_backward(inputs, grads_out, gate_w, up_w, down_w)
        summed = jnp.zeros((N_SP * CAP, D), jnp.float32)
        for part_index in range(N_TP):
            low_col = part_index * half_width
            partial_value = jnp.dot(gate_pre[:, low_col:low_col + half_width], gate_w[:, low_col:low_col + half_width].T, preferred_element_type=jnp.float32)
            partial_value = partial_value + jnp.dot(up_pre[:, low_col:low_col + half_width], up_w[:, low_col:low_col + half_width].T, preferred_element_type=jnp.float32)
            rounded = lax.optimization_barrier(partial_value.astype(jnp.bfloat16))
            summed = summed + rounded.astype(jnp.float32)
        return (gate_g, up_g, down_g, summed.astype(jnp.bfloat16))
    gate_grad, up_grad, down_grad, slot_grads = lax.map(one_expert, (table, gate_weight, up_weight, down_weight))
    token_index = (table.reshape(-1) // K).astype(jnp.int32)
    normed_grad = jnp.zeros((TOKENS + 1, D), jnp.float32).at[token_index].add(slot_grads.reshape(-1, D).astype(jnp.float32))[:TOKENS]
    cross = lax.optimization_barrier(jnp.sum(stream_float * norm_gain[None, :] * normed_grad, axis=1, keepdims=True))
    stream_grad = (cot_float + inverse * norm_gain[None, :] * normed_grad - stream_float * inverse * inverse * inverse * cross / D).astype(jnp.bfloat16)
    input_float = conv_input.astype(jnp.float32)
    cgate_float = conv_cgate.astype(jnp.float32)
    bgate_float = conv_bgate.astype(jnp.float32)
    gated = cgate_float * input_float
    padded = jnp.pad(gated, ((2, 0), (0, 0)))
    conv_out = conv_taps[0][None, :] * padded[:-2] + conv_taps[1][None, :] * padded[1:-1] + conv_taps[2][None, :] * padded[2:]
    mixer_out = (bgate_float * conv_out).astype(jnp.bfloat16)
    proj_grad = lax.dot_general(stream_grad, mixer_out, (((0,), (0,)), ((), ())), preferred_element_type=jnp.float32)
    mixer_grad = jnp.dot(stream_grad, out_proj, preferred_element_type=jnp.float32)
    delta = mixer_grad * bgate_float
    padded_back = jnp.pad(delta, ((0, 2), (0, 0)))
    gated_grad = conv_taps[2][None, :] * padded_back[:-2] + conv_taps[1][None, :] * padded_back[1:-1] + conv_taps[0][None, :] * padded_back[2:]
    bgate_grad = (mixer_grad * conv_out).astype(jnp.bfloat16)
    input_grad = (gated_grad * cgate_float).astype(jnp.bfloat16)
    cgate_grad = (gated_grad * input_float).astype(jnp.bfloat16)
    return (stream_grad, proj_grad, input_grad, bgate_grad, cgate_grad, gate_grad, up_grad, down_grad)
```

```python
import jax
import jax.numpy as jnp
from jax import lax
from jax.experimental import pallas as pl
from jax.experimental.pallas import tpu as pltpu
from jax.sharding import PartitionSpec as P

D = 2048


EPSILON = 1e-06


def shifted(value, axis, steps):
    count = lax.axis_size(axis)
    leading, last = (max(0, -steps), min(count, count - steps))
    return lax.ppermute(value, axis, [(source, source + steps) for source in range(leading, last)])


def slot_matrix(routes, experts, capacity):
    assigned = routes.reshape(-1)
    onehot = (assigned[:, None] == jnp.arange(experts, dtype=jnp.int32)[None, :]).astype(jnp.int32)
    earlier = jnp.cumsum(onehot, axis=0) - onehot
    position = jnp.sum(earlier * onehot, axis=1)
    target = assigned * capacity + position
    places = jnp.arange(experts * capacity, dtype=jnp.int32)
    return (places[:, None] == target[None, :]).astype(jnp.bfloat16)


def select_rows(selector, values):
    return jnp.dot(selector, values, preferred_element_type=jnp.float32).astype(jnp.bfloat16)


def contract_rows(left, right):
    return lax.dot_general(
        left, right, (((0,), (0,)), ((), ())), preferred_element_type=jnp.float32
    )


def contract_cols(left, right):
    return lax.dot_general(
        left, right, (((1,), (1,)), ((), ())), preferred_element_type=jnp.float32
    )


MESH = pl.DeviceIdType.MESH


def greet(count, peer_of, other=None):
    barrier = pltpu.get_barrier_semaphore()

    @pl.loop(1, count)
    def _(i):
        pl.semaphore_signal(barrier, inc=1, device_id={"sp": peer_of(i)}, device_id_type=MESH)

    if other is not None:
        pl.semaphore_signal(barrier, inc=1, device_id={"tp": other}, device_id_type=MESH)
    pl.semaphore_wait(barrier, count - 1 if other is None else count)


def dispatch_kernel(
    count,
    group,
    x_ref,
    y_ref,
    m_ref,
    ox_ref,
    oy_ref,
    om_ref,
    send,
    recv,
    fsend,
    frecv,
    msend,
    mrecv,
    own,
):
    me = lax.axis_index("sp")
    side = lax.axis_index("tp")
    other = 1 - side
    block = x_ref.shape[0] // count
    width = x_ref.shape[1]
    mine = pl.ds(pl.multiple_of(side * width, width), width)
    pairs = ((x_ref, ox_ref), (y_ref, oy_ref))

    def rows(index):
        return pl.ds(pl.multiple_of(index * block, block), block)

    def ahead(i):
        return i + side * (count - 2 * i)

    def remote(a, i):
        src, dst = pairs[a]
        peer = lax.rem(me + ahead(i), count)
        return pltpu.make_async_remote_copy(
            src_ref=src.at[rows(peer)],
            dst_ref=dst.at[rows(me), mine],
            send_sem=send.at[a, i],
            recv_sem=recv.at[a, i],
            device_id={"sp": peer},
            device_id_type=MESH,
        )

    def forward(a, i):
        dst = pairs[a][1]
        spot = dst.at[rows(lax.rem(me + count - ahead(i), count)), mine]
        return pltpu.make_async_remote_copy(
            src_ref=spot,
            dst_ref=spot,
            send_sem=fsend.at[a, i],
            recv_sem=frecv.at[a, i],
            device_id={"tp": other},
            device_id_type=MESH,
        )

    def home(a):
        src, dst = pairs[a]
        return pltpu.make_async_copy(src.at[rows(me)], dst.at[rows(me), mine], own.at[a])

    place = lax.rem(me, group)
    tokens = m_ref.shape[0]
    spot_m = om_ref.at[pl.ds(pl.multiple_of(place * tokens, tokens), tokens)]

    def mixer(i):
        return pltpu.make_async_remote_copy(
            src_ref=m_ref,
            dst_ref=spot_m,
            send_sem=msend.at[i],
            recv_sem=mrecv.at[i],
            device_id={"sp": me - place + lax.rem(place + i, group)},
            device_id_type=MESH,
        )

    home_m = pltpu.make_async_copy(m_ref, spot_m, own.at[2])
    greet(count, lambda i: lax.rem(me + i, count), other)
    for a in range(2):

        @pl.loop(1, count)
        def _(i):
            remote(a, i).start()

        home(a).start()

    @pl.loop(1, group)
    def _(i):
        mixer(i).start()

    home_m.start()
    for a in range(2):
        home(a).wait()
        forward(a, 0).start()

        @pl.loop(1, count)
        def _(i):
            remote(a, i).wait_recv()
            forward(a, i).start()

    for a in range(2):

        @pl.loop(1, count)
        def _(i):
            remote(a, i).wait_send()

        @pl.loop(0, count)
        def _(i):
            forward(a, i).wait()

    @pl.loop(1, group)
    def _(i):
        mixer(i).wait()

    home_m.wait()


def dispatch(x, y, mixed, group):
    count = lax.axis_size("sp")
    gathered = jax.ShapeDtypeStruct((group * mixed.shape[0], mixed.shape[1]), mixed.dtype)
    whole = jax.ShapeDtypeStruct((x.shape[0], 2 * x.shape[1]), x.dtype)
    return pl.pallas_call(
        lambda *refs: dispatch_kernel(count, group, *refs),
        out_shape=(whole, whole, gathered),
        in_specs=[pl.BlockSpec(memory_space=pltpu.VMEM)] * 3,
        out_specs=[pl.BlockSpec(memory_space=pltpu.VMEM)] * 3,
        scratch_shapes=[pltpu.SemaphoreType.DMA((2, count))] * 4
        + [pltpu.SemaphoreType.DMA((group,))] * 2
        + [pltpu.SemaphoreType.DMA((3,))],
        compiler_params=pltpu.CompilerParams(
            collective_id=0, has_side_effects=True, vmem_limit_bytes=40 * 2**20
        ),
        name="dispatch",
    )(x, y, mixed)


def spread_kernel(count, step, x_ref, o_ref, send, recv, own):
    me = lax.axis_index("sp")
    side = lax.axis_index("tp")
    here = lax.rem(lax.div(me, step), count)
    block = x_ref.shape[0] // count

    def rows(index):
        return pl.ds(pl.multiple_of(index * block, block), block)

    def slot(i):
        return lax.rem(here + i + side * (count - 2 * i), count)

    def peer_of(i):
        return me + (slot(i) - here) * step

    def remote(i):
        return pltpu.make_async_remote_copy(
            src_ref=x_ref.at[rows(slot(i))],
            dst_ref=o_ref.at[rows(here)],
            send_sem=send.at[i],
            recv_sem=recv.at[i],
            device_id={"sp": peer_of(i)},
            device_id_type=MESH,
        )

    greet(count, peer_of)

    @pl.loop(1, count)
    def _(i):
        remote(i).start()

    home = pltpu.make_async_copy(x_ref.at[rows(here)], o_ref.at[rows(here)], own)
    home.start()
    home.wait()

    @pl.loop(1, count)
    def _(i):
        remote(i).wait()


def spread(x, number, count, step):
    return pl.pallas_call(
        lambda *refs: spread_kernel(count, step, *refs),
        out_shape=jax.ShapeDtypeStruct(x.shape, x.dtype),
        in_specs=[pl.BlockSpec(memory_space=pltpu.VMEM)],
        out_specs=pl.BlockSpec(memory_space=pltpu.VMEM),
        scratch_shapes=[pltpu.SemaphoreType.DMA((count,))] * 2 + [pltpu.SemaphoreType.DMA],
        compiler_params=pltpu.CompilerParams(
            collective_id=number, has_side_effects=True, vmem_limit_bytes=24 * 2**20
        ),
        name="spread%d" % number,
    )(x)


def local(
    stream,
    norm_gain,
    cotangent,
    route_weights,
    routes,
    conv_input,
    conv_bgate,
    conv_cgate,
    conv_taps,
    out_proj,
    gate_weight,
    up_weight,
    down_weight,
):
    experts = lax.axis_size("sp")
    tok_count = stream.shape[0]
    top_count = routes.shape[1]
    capacity = 2 * tok_count * top_count // experts
    stream_float = stream.astype(jnp.float32)
    square_sum = lax.psum(jnp.sum(stream_float * stream_float, axis=1), "tp")
    inverse = lax.rsqrt(square_sum / D + EPSILON)[:, None]
    gain_row = norm_gain[None, :]
    normed = (stream_float * inverse * gain_row).astype(jnp.bfloat16)
    cot_float = cotangent.astype(jnp.float32)
    weighted = (route_weights[:, :, None] * cot_float[:, None, :]).astype(jnp.bfloat16)
    weighted = weighted.reshape(tok_count * top_count, -1)
    selector = slot_matrix(routes, experts, capacity)
    token_select = jnp.sum(selector.reshape(experts * capacity, tok_count, top_count), axis=2)
    send_inputs = select_rows(token_select, normed)
    send_grads = select_rows(selector, weighted)
    input_float = conv_input.astype(jnp.float32)
    cgate_float = conv_cgate.astype(jnp.float32)
    bgate_float = conv_bgate.astype(jnp.float32)
    rim_rows = shifted(jnp.stack([conv_input[-2:], conv_cgate[-2:]]), "sp", 1)
    rim_gated = rim_rows[1].astype(jnp.float32) * rim_rows[0].astype(jnp.float32)
    gated = cgate_float * input_float
    extended = jnp.concatenate([rim_gated, gated], axis=0)
    conv_out = (
        conv_taps[0][None, :] * extended[:-2]
        + conv_taps[1][None, :] * extended[1:-1]
        + conv_taps[2][None, :] * extended[2:]
    )
    mixer_out = (bgate_float * conv_out).astype(jnp.bfloat16)
    group = 2 ** ((experts.bit_length() - 1) // 2)
    stages = experts // group
    recv_inputs, recv_grads, mixer_near = dispatch(send_inputs, send_grads, mixer_out, group)
    gate_w = gate_weight[0]
    up_w = up_weight[0]
    down_w = down_weight[0]
    gate_lin = jnp.dot(recv_inputs, gate_w, preferred_element_type=jnp.float32)
    up_lin = jnp.dot(recv_inputs, up_w, preferred_element_type=jnp.float32)
    sigmoid_gate = jax.nn.sigmoid(gate_lin)
    silu_gate = gate_lin * sigmoid_gate
    hidden = (silu_gate * up_lin).astype(jnp.bfloat16)
    down_g = contract_rows(hidden, recv_grads)
    hidden_grad = contract_cols(recv_grads, down_w)
    gate_pre = (
        hidden_grad * up_lin * sigmoid_gate * (1.0 + gate_lin * (1.0 - sigmoid_gate))
    ).astype(jnp.bfloat16)
    up_pre = (hidden_grad * silu_gate).astype(jnp.bfloat16)
    gate_g = contract_rows(recv_inputs, gate_pre)
    up_g = contract_rows(recv_inputs, up_pre)
    side = lax.axis_index("tp")
    half = gate_w.shape[0] // 2

    def partial_of(part):
        gate_half = lax.dynamic_slice_in_dim(gate_w, part * half, half, axis=0)
        up_half = lax.dynamic_slice_in_dim(up_w, part * half, half, axis=0)
        value = contract_cols(gate_pre, gate_half) + contract_cols(up_pre, up_half)
        return lax.optimization_barrier(value.astype(jnp.bfloat16))

    theirs = lax.ppermute(partial_of(1 - side), "tp", [(0, 1), (1, 0)])
    summed = (partial_of(side).astype(jnp.float32) + theirs.astype(jnp.float32)).astype(
        jnp.bfloat16
    )
    returned = spread(summed, 1, experts, 1)
    normed_grad = contract_rows(token_select, returned)
    cross = lax.psum(jnp.sum(stream_float * gain_row * normed_grad, axis=1), "tp")
    stream_grad = (
        cot_float
        + inverse * gain_row * normed_grad
        - stream_float * inverse * inverse * inverse * cross[:, None] / D
    ).astype(jnp.bfloat16)
    grad_other = lax.ppermute(stream_grad, "tp", [(0, 1), (1, 0)])
    grad_whole = jnp.concatenate(
        [
            jnp.where(side == 0, stream_grad, grad_other),
            jnp.where(side == 0, grad_other, stream_grad),
        ],
        axis=1,
    )
    columns = grad_whole.reshape(tok_count, stages, group, -1).transpose(2, 0, 1, 3)
    grad_near = spread(columns.reshape(group * tok_count, -1), 2, group, 1)
    shares = contract_rows(grad_near, mixer_near).astype(jnp.bfloat16)
    shares = spread(shares, 3, stages, group)
    shares = shares.reshape(stages, shares.shape[0] // stages, -1)
    proj_grad = jnp.sum(shares.astype(jnp.float32), axis=0)
    mixer_grad = jnp.dot(grad_whole, out_proj, preferred_element_type=jnp.float32)
    delta = mixer_grad * bgate_float
    next_rim = shifted(delta[:2], "sp", -1)
    extended_back = jnp.concatenate([delta, next_rim], axis=0)
    gated_grad = (
        conv_taps[2][None, :] * extended_back[:-2]
        + conv_taps[1][None, :] * extended_back[1:-1]
        + conv_taps[0][None, :] * extended_back[2:]
    )
    bgate_grad = (mixer_grad * conv_out).astype(jnp.bfloat16)
    input_grad = (gated_grad * cgate_float).astype(jnp.bfloat16)
    cgate_grad = (gated_grad * input_float).astype(jnp.bfloat16)
    return (
        stream_grad,
        proj_grad,
        input_grad,
        bgate_grad,
        cgate_grad,
        gate_g[None],
        up_g[None],
        down_g[None],
    )


def solution(mesh):
    return jax.shard_map(
        local,
        mesh=mesh,
        in_specs=(
            P("sp", "tp"),
            P("tp"),
            P("sp", "tp"),
            P("sp", None),
            P("sp", None),
            P("sp", "tp"),
            P("sp", "tp"),
            P("sp", "tp"),
            P(None, "tp"),
            P(None, "tp"),
            P("sp", None, "tp"),
            P("sp", None, "tp"),
            P("sp", "tp", None),
        ),
        out_specs=(
            P("sp", "tp"),
            P("sp", "tp"),
            P("sp", "tp"),
            P("sp", "tp"),
            P("sp", "tp"),
            P("sp", None, "tp"),
            P("sp", None, "tp"),
            P("sp", "tp", None),
        ),
        check_vma=False,
    )
```
